32 devices in a mesh: sp: 4 (over z), fs: 4 (over y, x), tp: 2 (over core).
Axes of the slice: x: 2, y: 2, z: 4, core: 2. Of those that a mesh axis runs over, the one named last changes fastest.
Arguments:
- tokens: bfloat16 [4, 4096, 2048], P('fs', ('sp', 'tp')), may hold values from -6 to 6
- norm_gain: float32 [2048], replicated, may hold values from 0.1 to 1.9
- w_gate: bfloat16 [2048, 1024], P(('sp', 'fs'), 'tp'), may hold values from -0.125 to 0.125
- w_value: bfloat16 [2048, 1024], P(('sp', 'fs'), 'tp'), may hold values from -0.125 to 0.125
- w_bkey: bfloat16 [2048, 1024], P(('sp', 'fs'), 'tp'), may hold values from -0.125 to 0.125
- w_query: bfloat16 [2048, 1024], P(('sp', 'fs'), 'tp'), may hold values from -0.125 to 0.125
- w_pool_in: bfloat16 [2048, 1024], P(('sp', 'fs'), 'tp'), may hold values from -0.125 to 0.125
- w_step: bfloat16 [2048, 2, 16], replicated, may hold values from -0.125 to 0.125
- step_bias: float32 [2, 16], replicated, may hold values from -1 to 1
- decay_rate: float32 [2, 16], replicated, may hold values from 4.8828125e-06 to 0.06
- decay_shift: float32 [4, 16, 2, 4096], P('fs', 'tp', None, 'sp'), may hold values from 0 to 2.2
- conv_value: bfloat16 [5, 1024], replicated, may hold values from -2.5 to 2.5
- conv_bkey: bfloat16 [5, 1024], replicated, may hold values from -2.5 to 2.5
- conv_query: bfloat16 [5, 1024], replicated, may hold values from -2.5 to 2.5
- mix_gain: float32 [1024], replicated, may hold values from 0.1 to 1.9
- pool_mix: bfloat16 [8, 128, 128], replicated, may hold values from -0.5 to 0.5
- pool_gain: float32 [1024], replicated, may hold values from 0.1 to 1.9
- w_out_ssd: bfloat16 [1024, 2048], P('tp', ('sp', 'fs')), may hold values from -0.125 to 0.125
- w_out_pool: bfloat16 [1024, 2048], P('tp', ('sp', 'fs')), may hold values from -0.125 to 0.125
Outputs:
- mixed: bfloat16 [4, 4096, 2048], P('fs', ('sp', 'tp'))
The draws below stay inside these ranges and needn't reach their ends.
All inputs are finite; a program needn't handle non-finite values.
Results may differ from the reference program's by a relative error of at most 0.014.
Values may be sent and summed in bfloat16 or wider, within the bound.
No kernel may reach another device: no remote copies, remote signals or barrier semaphores. Data moves between devices by JAX's collectives and lax.ppermute only.
A program may use at most 128 MiB of HBM per device.

```python
import jax
import jax.numpy as jnp
from jax import lax

D = 2048
HEAD_DIM = 64
DUALITY_HEADS = 16
GROUPS = 8
STATE = 128
CONV_WIDTH = 5
POOL_GROUPS = 8
POOL_DIM = 128
SPAN = 128
TOK_SP = 1024
SEQUENCE_LENGTH = 4096
BATCH_SEQUENCES = 4
D_SSM = 1024
D_POOL = 1024
N_TP = 2


def draw_decay_rate(key, part):
    order_key, slow_key, fast_key = jax.random.split(jax.random.fold_in(key, 11), 3)
    ranking = jax.random.permutation(order_key, 2 * DUALITY_HEADS)
    slow_count = DUALITY_HEADS
    slow_rate = jax.random.uniform(slow_key, (2 * DUALITY_HEADS,), jnp.float32, 0.02, 0.2) / SEQUENCE_LENGTH
    fast_rate = jax.random.uniform(fast_key, (2 * DUALITY_HEADS,), jnp.float32, 0.02, 0.06)
    rates = jnp.where(ranking < slow_count, slow_rate, fast_rate)
    return rates.reshape(2, DUALITY_HEADS).astype(jnp.float32)


def draw_decay_shift(key, part):
    random_keys = jax.random.split(jax.random.fold_in(key, 23), 4)
    token_position = jnp.arange(SEQUENCE_LENGTH, dtype=jnp.int32)
    segment = token_position // TOK_SP
    segments = SEQUENCE_LENGTH // TOK_SP
    low_end, high_end = (0.4, 2.5)
    factor = jnp.exp(jax.random.uniform(random_keys[0], (BATCH_SEQUENCES, DUALITY_HEADS, 2, segments), jnp.float32, jnp.log(low_end), jnp.log(high_end)))
    roughness = jax.random.uniform(random_keys[1], (BATCH_SEQUENCES, DUALITY_HEADS, 2, SEQUENCE_LENGTH), jnp.float32, 0.5, 1.5)
    reference_level = jnp.take(factor, segment, axis=3) * roughness * (0.3 / SEQUENCE_LENGTH)
    spike_places = jax.random.randint(random_keys[2], (BATCH_SEQUENCES, DUALITY_HEADS, 2, 3), 0, SEQUENCE_LENGTH)
    spike_length = jax.random.uniform(random_keys[3], (BATCH_SEQUENCES, DUALITY_HEADS, 2, 3), jnp.float32, 0.22, 0.69)
    match_count = (token_position[None, None, None, None, :] == spike_places[..., None]).astype(jnp.float32)
    spike_runs = jnp.sum(match_count * spike_length[..., None], axis=3)
    return (reference_level + spike_runs).astype(jnp.float32)


def levels(stream_key, shape, pieces, low, top_value):
    loudness = 1.0
    for dim, parts in pieces:
        steps = jax.random.uniform(jax.random.fold_in(jax.random.fold_in(stream_key, 6), dim), (parts,), jnp.float32, low / len(pieces), top_value / len(pieces))
        loudness = loudness * jnp.repeat(jnp.exp(steps), shape[dim] // parts).reshape((-1,) + (1,) * (len(shape) - 1 - dim))
    return loudness


def gaussian(own_key, extent, deviation, bound, cuts=(), held_as=jnp.bfloat16):
    array = deviation * jax.random.normal(own_key, extent, jnp.float32)
    if cuts:
        array = array * levels(own_key, extent, cuts, -0.22, 0.18)
    return jnp.clip(array, -bound, bound).astype(held_as)


def setup_inputs(seed: int = 0) -> dict:
    splits = jax.random.split(jax.random.key(seed), 20)
    tokens = gaussian(splits[0], (BATCH_SEQUENCES, SEQUENCE_LENGTH, D), 1.0, 6.0, ((0, 4), (1, 8)))
    norm_gain = jnp.clip(1.0 + 0.18 * jax.random.normal(splits[1], (D,), jnp.float32), 0.1, 1.9)
    w_gate = gaussian(splits[2], (D, D_SSM), D ** -0.5, 0.125, ((0, 16), (1, 2)))
    w_value = gaussian(splits[3], (D, D_SSM), D ** -0.5, 0.125, ((0, 16), (1, 2)))
    w_bkey = gaussian(splits[4], (D, GROUPS * STATE), D ** -0.5, 0.125, ((0, 16), (1, 2)))
    w_query = gaussian(splits[5], (D, GROUPS * STATE), D ** -0.5, 0.125, ((0, 16), (1, 2)))
    w_pool_in = gaussian(splits[6], (D, D_POOL), D ** -0.5, 0.125, ((0, 16), (1, 2)))
    w_step = gaussian(splits[7], (D, 2, DUALITY_HEADS), D ** -0.5, 0.125)
    step_bias = jnp.clip(jax.random.uniform(splits[8], (2, DUALITY_HEADS), jnp.float32, -1.0, 1.0), -1.0, 1.0)
    decay_rate = draw_decay_rate(jax.random.fold_in(splits[19], 71), 0)
    decay_shift = draw_decay_shift(jax.random.fold_in(splits[19], 71), 0)
    conv_value = gaussian(splits[11], (CONV_WIDTH, D_SSM), CONV_WIDTH ** -0.5, 2.5)
    conv_bkey = gaussian(splits[12], (CONV_WIDTH, GROUPS * STATE), CONV_WIDTH ** -0.5, 2.5)
    conv_query = gaussian(splits[13], (CONV_WIDTH, GROUPS * STATE), CONV_WIDTH ** -0.5, 2.5)
    mix_gain = jnp.clip(1.0 + 0.18 * jax.random.normal(splits[14], (D_SSM,), jnp.float32), 0.1, 1.9)
    pool_mix = gaussian(splits[15], (POOL_GROUPS, POOL_DIM, POOL_DIM), POOL_DIM ** -0.5, 0.5)
    pool_gain = jnp.clip(1.0 + 0.18 * jax.random.normal(splits[16], (D_POOL,), jnp.float32), 0.1, 1.9)
    w_out_ssd = gaussian(splits[17], (D_SSM, D), (D_SSM + D_POOL) ** -0.5, 0.125, ((0, 2), (1, 16)))
    w_out_pool = gaussian(splits[18], (D_POOL, D), (D_SSM + D_POOL) ** -0.5, 0.125, ((0, 2), (1, 16)))
    return {"tokens": tokens, "norm_gain": norm_gain, "w_gate": w_gate, "w_value": w_value, "w_bkey": w_bkey, "w_query": w_query, "w_pool_in": w_pool_in, "w_step": w_step, "step_bias": step_bias, "decay_rate": decay_rate, "decay_shift": decay_shift, "conv_value": conv_value, "conv_bkey": conv_bkey, "conv_query": conv_query, "mix_gain": mix_gain, "pool_mix": pool_mix, "pool_gain": pool_gain, "w_out_ssd": w_out_ssd, "w_out_pool": w_out_pool}


EPSILON = 1e-06
HIGHEST = lax.Precision.HIGHEST
WINDOWS = (2, 4, 8, 16)

def blockwise(values, bkeys, queries, steps, logs):
    length, heads, head_width = values.shape
    groups, state_width = (bkeys.shape[1], bkeys.shape[2])
    per_group = heads // groups
    blocks = length // SPAN
    weighted = (values * jnp.transpose(steps)[:, :, None]).reshape(blocks, SPAN, groups, per_group, head_width)
    key_blocks = bkeys.reshape(blocks, SPAN, groups, state_width)
    query_blocks = queries.reshape(blocks, SPAN, groups, state_width)
    inner = jnp.cumsum(logs.reshape(heads, blocks, SPAN), axis=-1)
    lower = jnp.tril(jnp.ones((SPAN, SPAN), dtype=bool))
    within = jnp.exp(jnp.where(lower, inner[..., :, None] - inner[..., None, :], -jnp.inf))
    within = within.reshape(groups, per_group, blocks, SPAN, SPAN)
    scores = jnp.einsum('clgn,csgn->cgls', query_blocks, key_blocks, precision=HIGHEST)
    diagonal = jnp.einsum('cgls,gkcls,csgkp->clgkp', scores, within, weighted, precision=HIGHEST)
    tails = jnp.exp(inner[..., -1:] - inner).reshape(groups, per_group, blocks, SPAN)
    ends = jnp.einsum('clgn,gkcl,clgkp->cgkpn', key_blocks, tails, weighted, precision=HIGHEST)
    totals = inner[..., -1]
    upto = jnp.cumsum(totals, axis=-1)
    before = upto - totals
    block_ids = jnp.arange(blocks, dtype=jnp.int32)
    earlier = block_ids[None, :] < block_ids[:, None]
    between = jnp.exp(jnp.where(earlier[None], before[:, :, None] - upto[:, None, :], -jnp.inf))
    between = between.reshape(groups, per_group, blocks, blocks)
    prior = jnp.einsum('gkcj,jgkpn->cgkpn', between, ends, precision=HIGHEST)
    reach = jnp.exp(inner).reshape(groups, per_group, blocks, SPAN)
    offdiag = jnp.einsum('clgn,cgkpn,gkcl->clgkp', query_blocks, prior, reach, precision=HIGHEST)
    return (diagonal + offdiag).reshape(length, heads, head_width)

def centred(projected, taps):
    margin = CONV_WIDTH // 2
    length = projected.shape[0]
    padded = jnp.pad(projected, ((margin, margin), (0, 0)))
    running = jnp.zeros(projected.shape, jnp.float32)
    for offset in range(CONV_WIDTH):
        running = running + padded[offset:offset + length].astype(jnp.float32) * taps[offset].astype(jnp.float32)
    return running

def box_mean(column, window):
    length = column.shape[0]
    prefix = jnp.pad(jnp.cumsum(column, axis=0), ((1, 0), (0, 0)))
    where_now = jnp.arange(length, dtype=jnp.int32)
    lower = jnp.clip(where_now - window // 2, 0, length).astype(jnp.int32)
    upper = jnp.clip(where_now + window - window // 2, 0, length).astype(jnp.int32)
    counts = (upper - lower).astype(jnp.float32)
    return (prefix[upper] - prefix[lower]) / counts[:, None]

def reference(tokens, norm_gain, w_gate, w_value, w_bkey, w_query, w_pool_in, w_step, step_bias, decay_rate, decay_shift, conv_value, conv_bkey, conv_query, mix_gain, pool_mix, pool_gain, w_out_ssd, w_out_pool):

    def one_sequence(paired):
        rows, shift = paired
        length = rows.shape[0]
        widened = rows.astype(jnp.float32)
        normed = (widened * lax.rsqrt(lax.optimization_barrier(jnp.mean(widened * widened, axis=-1, keepdims=True)) + EPSILON) * norm_gain).astype(jnp.bfloat16)
        gate = jnp.dot(normed, w_gate, preferred_element_type=jnp.float32).astype(jnp.bfloat16)
        value = jnp.dot(normed, w_value, preferred_element_type=jnp.float32).astype(jnp.bfloat16)
        bkey = jnp.dot(normed, w_bkey, preferred_element_type=jnp.float32).astype(jnp.bfloat16)
        query = jnp.dot(normed, w_query, preferred_element_type=jnp.float32).astype(jnp.bfloat16)
        pooled = jnp.dot(normed, w_pool_in, preferred_element_type=jnp.float32).astype(jnp.bfloat16)
        raw_steps = jnp.dot(normed, w_step.reshape(D, 2 * DUALITY_HEADS), preferred_element_type=jnp.float32)
        steps = jax.nn.softplus(raw_steps.reshape(length, 2, DUALITY_HEADS) + step_bias).transpose(1, 2, 0)
        logs = -decay_rate[:, :, None] * steps - shift.transpose(1, 0, 2)
        values = jax.nn.silu(centred(value, conv_value)).reshape(length, DUALITY_HEADS, HEAD_DIM)
        bkeys = jax.nn.silu(centred(bkey, conv_bkey)).reshape(length, GROUPS, STATE)
        queries = jax.nn.silu(centred(query, conv_query)).reshape(length, GROUPS, STATE)
        forward = blockwise(values, bkeys, queries, steps[0], logs[0])
        backward = blockwise(values[::-1], bkeys[::-1], queries[::-1], steps[1][:, ::-1], logs[1][:, ::-1])[::-1]
        heads_out = forward + backward
        gated = heads_out.reshape(length, D_SSM) * jax.nn.silu(gate.astype(jnp.float32))
        ssd_mix = (gated * lax.rsqrt(lax.optimization_barrier(jnp.mean(gated * gated, axis=-1, keepdims=True)) + EPSILON) * mix_gain).astype(jnp.bfloat16)
        pool_rows = pooled.astype(jnp.float32).reshape(length, POOL_GROUPS, POOL_DIM)
        differences = []
        for group in range(POOL_GROUPS):
            column = pool_rows[:, group]
            differences.append(box_mean(column, WINDOWS[group % 4]) - column)
        pool_diff = jnp.stack(differences, axis=1).astype(jnp.bfloat16)
        mapped = jnp.einsum('sgc,gcd->sgd', pool_diff.astype(jnp.float32), pool_mix.astype(jnp.float32))
        pool_out = (mapped.reshape(length, D_POOL) * pool_gain).astype(jnp.bfloat16)
        ssd_part = D_SSM // N_TP
        pool_part = D_POOL // N_TP
        summed = jnp.zeros((length, D), jnp.float32)
        for member in range(N_TP):
            partial_value = jnp.dot(ssd_mix[:, member * ssd_part:(member + 1) * ssd_part], w_out_ssd[member * ssd_part:(member + 1) * ssd_part], preferred_element_type=jnp.float32)
            partial_value = partial_value + jnp.dot(pool_out[:, member * pool_part:(member + 1) * pool_part], w_out_pool[member * pool_part:(member + 1) * pool_part], preferred_element_type=jnp.float32)
            rounded = lax.optimization_barrier(partial_value.astype(jnp.bfloat16))
            summed = summed + rounded.astype(jnp.float32)
        return summed.astype(jnp.bfloat16)
    return lax.map(one_sequence, (tokens, decay_shift))
```

```python
import functools

import jax
import jax.numpy as jnp
from jax import lax
from jax.experimental import pallas as pl
from jax.experimental.pallas import tpu as pltpu
from jax.sharding import PartitionSpec as P

HEAD_DIM = 64
DUALITY_HEADS = 16
GROUPS = 8
STATE = 128
CONV_WIDTH = 5
POOL_GROUPS = 8
POOL_DIM = 128
SPAN = 128
REACH = 8
D_SSM = 1024
EPSILON = 1e-06
HIGHEST = lax.Precision.HIGHEST
WINDOWS = (2, 4, 8, 16)
F32 = jnp.float32
BF16 = jnp.bfloat16

VMEM_LIMIT = 56 * 1024 * 1024


def row_chunk(rows):
    for size in range(256, 15, -16):
        if rows % size == 0:
            return size
    return rows


def ring_blocks(block):
    count = lax.axis_size("sp")
    return [block] + [
        lax.ppermute(block, "sp", [(i, (i + k) % count) for i in range(count)])
        for k in range(1, count)
    ]


def cube_pair(stacked, bits):
    count = lax.axis_size("fs")
    for place, bit in enumerate(bits):
        other = lax.ppermute(stacked, "fs", [(i, i ^ bit) for i in range(count)])
        if place == len(bits) - 1:
            return stacked, other
        stacked = jnp.concatenate([stacked, other], axis=0)


def piece_sources(bits):
    sp_count, fs_count = lax.axis_size("sp"), lax.axis_size("fs")
    sp_rank, fs_rank = lax.axis_index("sp"), lax.axis_index("fs")
    sources = []
    for step in range(fs_count):
        fs_from = fs_rank
        for place, bit in enumerate(bits):
            if step >> place & 1:
                fs_from = fs_from ^ bit
        for back in range(sp_count):
            sources.append((sp_rank - back + sp_count) % sp_count * fs_count + fs_from)
    return jnp.stack(sources).astype(jnp.int32)


def gather_two(first, second):
    fs_count = lax.axis_size("fs")
    bits = [1 << n for n in range(fs_count.bit_length() - 1)]
    blocks = ring_blocks(jnp.stack([first, second]))
    one = cube_pair(jnp.stack([b[0] for b in blocks]), bits)
    two = cube_pair(jnp.stack([b[1] for b in blocks]), bits[::-1])
    return one, two


def start_copies(index_ref, refs, target, sems, place):
    copies = []
    for ref in refs:
        for piece in range(ref.shape[0]):
            where = place(index_ref[len(copies)])
            copy = pltpu.make_async_copy(ref.at[piece], target.at[where], sems.at[len(copies)])
            copy.start()
            copies.append(copy)
    return copies


def rows_at(height, shift=0, stride=None):
    stride = height if stride is None else stride

    def place(index):
        return (pl.ds(pl.multiple_of(index * stride + shift, 16), height), slice(None))

    return place


def columns_at(width):
    def place(index):
        return (slice(None), pl.ds(pl.multiple_of(index * width, 128), width))

    return place


def project_into(normed_ref, weight, scratch):
    rows = normed_ref.shape[0]
    chunk = row_chunk(rows)

    def step(i, carry):
        at = pl.ds(pl.multiple_of(i * chunk, 16), chunk)
        product = jnp.dot(normed_ref[at, :], weight[...], preferred_element_type=F32)
        scratch[at, :] = product.astype(BF16).astype(F32)
        return carry

    lax.fori_loop(0, rows // chunk, step, 0)


def fill_weight(index_refs, piece_refs, weight, sems, whole_height):
    copies = []
    shift = 0
    for n, (index_ref, refs) in enumerate(zip(index_refs, piece_refs)):
        height = refs[0].shape[1]
        copies += start_copies(
            index_ref, refs, weight, sems.at[n], rows_at(height, shift, whole_height)
        )
        shift += height
    for copy in copies:
        copy.wait()


def conv_kernel(n_parts, *refs):
    indexes = refs[:n_parts]
    normed_ref, taps_ref = refs[n_parts], refs[n_parts + 1]
    pieces = refs[n_parts + 2 : 3 * n_parts + 2]
    out_ref, weight, scratch, sems = refs[3 * n_parts + 2 :]
    pairs = [pieces[2 * n : 2 * n + 2] for n in range(n_parts)]
    height = sum(p[0].shape[1] for p in pairs)
    fill_weight(indexes, pairs, weight, sems, height)
    project_into(normed_ref, weight, scratch)
    span = SPAN
    margin = CONV_WIDTH // 2
    tall = span + 2 * REACH

    def step(i, carry):
        window = scratch[pl.ds(pl.multiple_of(i * span, 8), tall), :]
        total = window * taps_ref[margin : margin + 1, :]
        for tap in range(CONV_WIDTH):
            if tap != margin:
                turned = pltpu.roll(window, (margin - tap) % tall, 0)
                total = total + turned * taps_ref[tap : tap + 1, :]
        total = total[REACH : REACH + span]
        out_ref[pl.ds(pl.multiple_of(i * span, 16), span), :] = jax.nn.silu(total).astype(BF16)
        return carry

    lax.fori_loop(0, out_ref.shape[0] // span, step, 0)


def gate_kernel(index, normed_ref, first, second, out_ref, weight, sems):
    fill_weight([index], [(first, second)], weight, sems, first.shape[1])
    length = out_ref.shape[0]
    chunk = row_chunk(length)

    def step(i, carry):
        at = pl.ds(pl.multiple_of(REACH + i * chunk, 8), chunk)
        to = pl.ds(pl.multiple_of(i * chunk, 16), chunk)
        product = jnp.dot(normed_ref[at, :], weight[...], preferred_element_type=F32)
        out_ref[to, :] = product.astype(BF16)
        return carry

    lax.fori_loop(0, length // chunk, step, 0)


def pool_kernel(
    index, where, normed_ref, first, second, mix_ref, gain_ref, out_ref, weight, scratch, sems
):
    fill_weight([index], [(first, second)], weight, sems, first.shape[1])
    project_into(normed_ref, weight, scratch)
    length, width = out_ref.shape
    pools = width // POOL_DIM
    tall = SPAN + 2 * REACH

    def step(i, carry):
        base = where[0] + i * SPAN
        at = pl.ds(pl.multiple_of(i * SPAN, 8), tall)
        position = base - REACH + lax.broadcasted_iota(jnp.int32, (tall, POOL_DIM), 0)
        for pool in range(pools):
            lanes = slice(pool * POOL_DIM, (pool + 1) * POOL_DIM)
            window = scratch[at, lanes]
            sums = [window + pltpu.roll(window, 1, 0)]
            for half in (1, 2, 4):
                last = sums[-1]
                sums.append(pltpu.roll(last, half, 0) + pltpu.roll(last, tall - half, 0))
            means = []
            for size, total in zip(WINDOWS, sums):
                lower = jnp.clip(position - size // 2, 0, where[1])
                upper = jnp.clip(position + size - size // 2, 0, where[1])
                count = jnp.maximum(upper - lower, 1).astype(F32)
                means.append(functools.partial(jnp.divide, total, count))
            if pools % len(WINDOWS) == 0:
                mean = means[pool % len(WINDOWS)]()
            else:
                kind = (where[2] + pool) % len(WINDOWS)
                mean = means[0]()
                for n in range(1, len(WINDOWS)):
                    mean = jnp.where(kind == n, means[n](), mean)
            gap = (mean - window)[REACH : REACH + SPAN].astype(BF16)
            mapped = jnp.dot(gap, mix_ref[pool], preferred_element_type=F32)
            to = pl.ds(pl.multiple_of(i * SPAN, 16), SPAN)
            out_ref[to, lanes] = (mapped * gain_ref[:, lanes]).astype(BF16)
        return carry

    lax.fori_loop(0, length // SPAN, step, 0)


def spread(columns, first, per_group):
    rows = columns.shape[0]
    wide = [
        jnp.broadcast_to(columns[:, first + k : first + k + 1], (rows, HEAD_DIM))
        for k in range(per_group)
    ]
    return jnp.concatenate(wide, axis=1)


def state_kernel(keys_ref, values_ref, columns_ref, decay_ref, prior_ref, final_ref, ends):
    length = keys_ref.shape[0]
    blocks = length // SPAN
    half = values_ref.shape[1]
    per_group = half // HEAD_DIM
    for c in range(blocks):
        at = slice(c * SPAN, (c + 1) * SPAN)
        value = values_ref[at, :].astype(F32)
        columns = columns_ref[0, at, :]
        weighted = jnp.concatenate(
            [value * spread(columns, 0, per_group), value * spread(columns, per_group, per_group)],
            axis=1,
        ).astype(BF16)
        ends[c] = lax.dot_general(
            keys_ref[at, :], weighted, (((0,), (0,)), ((), ())), preferred_element_type=F32
        )
    state = jnp.zeros((STATE, half), F32)
    for c in range(blocks):
        prior_ref[c, 0, :, :half] = state.astype(BF16)
        state = state * decay_ref[0, c : c + 1, :half] + ends[c, :, :half]
    final_ref[0, 0] = state
    state = jnp.zeros((STATE, half), F32)
    for c in range(blocks - 1, -1, -1):
        prior_ref[c, 0, :, half:] = state.astype(BF16)
        state = state * decay_ref[0, c : c + 1, half:] + ends[c, :, half:]
    final_ref[1, 0] = state


def mixer_kernel(
    heads,
    queries_ref,
    keys_ref,
    values_ref,
    gate_ref,
    prior_ref,
    forward_ref,
    backward_ref,
    entry_ref,
    columns_ref,
    rows_ref,
    gain_ref,
    out_ref,
    squares_ref,
):
    width = values_ref.shape[1]
    groups = queries_ref.shape[1] // STATE
    per_group = heads // groups
    half = per_group * HEAD_DIM
    line = lax.broadcasted_iota(jnp.int32, (SPAN, SPAN), 0)
    lane = lax.broadcasted_iota(jnp.int32, (SPAN, SPAN), 1)
    later = line >= lane
    same = line == lane
    head_of = lax.broadcasted_iota(jnp.int32, (SPAN, half), 1) // HEAD_DIM
    columns = columns_ref[...]
    squares = jnp.zeros((SPAN, 1), F32)
    for g in range(groups):
        states = slice(g * STATE, (g + 1) * STATE)
        lanes = slice(g * half, (g + 1) * half)
        query = queries_ref[:, states]
        value = values_ref[:, lanes]
        scores = lax.dot_general(
            query, keys_ref[:, states], (((1,), (1,)), ((), ())), preferred_element_type=F32
        )
        parts, stacked = [], []
        for k in range(per_group):
            h = g * per_group + k
            ahead_c = columns[:, h : h + 1]
            back_c = columns[:, heads + h : heads + h + 1]
            ahead_r = rows_ref[h : h + 1, :]
            back_r = rows_ref[heads + h : heads + h + 1, :]
            step_f = rows_ref[2 * heads + h : 2 * heads + h + 1, :]
            step_b = rows_ref[3 * heads + h : 3 * heads + h + 1, :]
            decay = jnp.exp(jnp.where(later, ahead_c - ahead_r, back_r - back_c))
            weight = jnp.where(later, step_f, step_b) + jnp.where(same, step_b, 0.0)
            parts.append((scores * decay * weight).astype(BF16))
            stacked.append(jnp.where(head_of == k, value, jnp.zeros_like(value)))
        result = jnp.dot(
            jnp.concatenate(parts, axis=1),
            jnp.concatenate(stacked, axis=0),
            preferred_element_type=F32,
        )
        carried = jnp.concatenate([forward_ref[g], backward_ref[g]], axis=1)
        state = prior_ref[0, g].astype(F32) + carried * entry_ref[0, g : g + 1, :]
        away = jnp.dot(query, state.astype(BF16), preferred_element_type=F32)
        result = result + away[:, :half] * spread(columns, 2 * heads + g * per_group, per_group)
        result = result + away[:, half:] * spread(columns, 3 * heads + g * per_group, per_group)
        gated = result * jax.nn.silu(gate_ref[:, lanes].astype(F32))
        squares = squares + jnp.sum(gated * gated, axis=1, keepdims=True)
        out_ref[:, lanes] = (gated * gain_ref[:, lanes]).astype(BF16)
    squares_ref[...] = squares


def output_kernel(
    index_a,
    index_b,
    start,
    mix_ref,
    pool_ref,
    scale_ref,
    *refs,
):
    del start
    pieces_a, pieces_b = refs[: len(refs) // 2 - 2], refs[len(refs) // 2 - 2 : -4]
    out_ref, weight_a, weight_b, sems = refs[-4:]

    @pl.when(pl.program_id(0) == 0)
    def _():
        step = columns_at(pieces_a[0].shape[2])
        copies = start_copies(index_a, pieces_a, weight_a, sems.at[0], step)
        copies += start_copies(index_b, pieces_b, weight_b, sems.at[1], step)
        for copy in copies:
            copy.wait()

    first = jnp.dot(mix_ref[...], weight_a[...], preferred_element_type=F32)
    second = jnp.dot(pool_ref[...], weight_b[...], preferred_element_type=F32)
    out_ref[...] = (first * scale_ref[...] + second).astype(BF16)


def any_spec():
    return pl.BlockSpec(memory_space=pl.ANY)


def params(grid_dims=0):
    return pltpu.CompilerParams(
        vmem_limit_bytes=VMEM_LIMIT,
        dimension_semantics=("arbitrary",) * grid_dims if grid_dims else None,
    )


def cost(flops, nbytes=0):
    return pl.CostEstimate(flops=int(flops), bytes_accessed=int(nbytes), transcendentals=0)


def whole(shape):
    return pl.BlockSpec(shape, lambda *_: (0,) * len(shape))


def smem():
    return pl.BlockSpec(memory_space=pltpu.SMEM)


def convolved(normed, taps, indexes, pairs, name):
    rows, depth = normed.shape
    width = pairs[0][0].shape[-1]
    n_parts = len(pairs)
    pieces = [p for pair in pairs for p in pair]
    count = 2 * pieces[0].shape[0]
    return pl.pallas_call(
        functools.partial(conv_kernel, n_parts),
        out_shape=jax.ShapeDtypeStruct((rows - 2 * REACH, width), BF16),
        in_specs=[smem()] * n_parts
        + [pl.BlockSpec(memory_space=pltpu.VMEM)] * 2
        + [any_spec()] * len(pieces),
        out_specs=pl.BlockSpec(memory_space=pltpu.VMEM),
        scratch_shapes=[
            pltpu.VMEM((depth, width), BF16),
            pltpu.VMEM((rows, width), F32),
            pltpu.SemaphoreType.DMA((n_parts, count)),
        ],
        compiler_params=params(),
        cost_estimate=cost(2 * rows * depth * width),
        name=name,
    )(*indexes, normed, taps, *pieces)


def gate_projection(normed, index, pair):
    rows, depth = normed.shape
    width = pair[0].shape[-1]
    return pl.pallas_call(
        gate_kernel,
        out_shape=jax.ShapeDtypeStruct((rows - 2 * REACH, width), BF16),
        in_specs=[smem(), pl.BlockSpec(memory_space=pltpu.VMEM), any_spec(), any_spec()],
        out_specs=pl.BlockSpec(memory_space=pltpu.VMEM),
        scratch_shapes=[
            pltpu.VMEM((depth, width), BF16),
            pltpu.SemaphoreType.DMA((1, 2 * pair[0].shape[0])),
        ],
        compiler_params=params(),
        cost_estimate=cost(2 * rows * depth * width),
        name="gate_proj",
    )(index, normed, *pair)


def pool_branch(normed, index, pair, where, mix, gain):
    rows, depth = normed.shape
    width = pair[0].shape[-1]
    vmem = pl.BlockSpec(memory_space=pltpu.VMEM)
    return pl.pallas_call(
        pool_kernel,
        out_shape=jax.ShapeDtypeStruct((rows - 2 * REACH, width), BF16),
        in_specs=[smem(), smem(), vmem, any_spec(), any_spec(), vmem, vmem],
        out_specs=vmem,
        scratch_shapes=[
            pltpu.VMEM((depth, width), BF16),
            pltpu.VMEM((rows, width), F32),
            pltpu.SemaphoreType.DMA((1, 2 * pair[0].shape[0])),
        ],
        compiler_params=params(),
        cost_estimate=cost(2 * rows * depth * width),
        name="pool_branch",
    )(index, where, normed, *pair, mix, gain)


def block_states(keys, values, columns, decay):
    length = keys.shape[0]
    groups = keys.shape[1] // STATE
    half = values.shape[1] // groups
    blocks = length // SPAN
    return pl.pallas_call(
        state_kernel,
        grid=(groups,),
        out_shape=(
            jax.ShapeDtypeStruct((blocks, groups, STATE, 2 * half), BF16),
            jax.ShapeDtypeStruct((2, groups, STATE, half), F32),
        ),
        in_specs=[
            pl.BlockSpec((length, STATE), lambda g: (0, g)),
            pl.BlockSpec((length, half), lambda g: (0, g)),
            pl.BlockSpec((1, length, columns.shape[2]), lambda g: (g, 0, 0)),
            pl.BlockSpec((1, blocks, 2 * half), lambda g: (g, 0, 0)),
        ],
        out_specs=(
            pl.BlockSpec((blocks, 1, STATE, 2 * half), lambda g: (0, g, 0, 0)),
            pl.BlockSpec((2, 1, STATE, half), lambda g: (0, g, 0, 0)),
        ),
        scratch_shapes=[pltpu.VMEM((blocks, STATE, 2 * half), F32)],
        compiler_params=params(1),
        cost_estimate=cost(1e9),
        name="block_states",
    )(keys, values, columns, decay)


def mixed_heads(
    queries, keys, values, gate, prior, forward, backward, entry, columns, rows, gain, heads
):
    length, width = values.shape
    groups = queries.shape[1] // STATE
    half = width // groups
    blocks = length // SPAN
    tall = pl.BlockSpec((SPAN, width), lambda c: (c, 0))
    state = pl.BlockSpec((SPAN, groups * STATE), lambda c: (c, 0))
    return pl.pallas_call(
        functools.partial(mixer_kernel, heads),
        grid=(blocks,),
        out_shape=(
            jax.ShapeDtypeStruct((length, width), BF16),
            jax.ShapeDtypeStruct((length, 1), F32),
        ),
        in_specs=[
            state,
            state,
            tall,
            tall,
            pl.BlockSpec((1, groups, STATE, 2 * half), lambda c: (c, 0, 0, 0)),
            whole(forward.shape),
            whole(backward.shape),
            pl.BlockSpec((1, groups, 2 * half), lambda c: (c, 0, 0)),
            pl.BlockSpec((SPAN, columns.shape[1]), lambda c: (c, 0)),
            pl.BlockSpec((rows.shape[0], SPAN), lambda c: (0, c)),
            whole(gain.shape),
        ],
        out_specs=(tall, pl.BlockSpec((SPAN, 1), lambda c: (c, 0))),
        compiler_params=params(1),
        cost_estimate=cost(2e9),
        name="mixed_heads",
    )(queries, keys, values, gate, prior, forward, backward, entry, columns, rows, gain)


def output_rows(mix, pool, scale, index_a, index_b, pair_a, pair_b, start, count, name):
    width = mix.shape[1]
    pieces = sum(p.shape[0] for p in pair_a)
    cols = pieces * pair_a[0].shape[2]
    block = min(count, 256)
    row_map = lambda i, ia, ib, s: (s[0] + i, 0)
    return pl.pallas_call(
        output_kernel,
        grid_spec=pltpu.PrefetchScalarGridSpec(
            num_scalar_prefetch=3,
            grid=(count // block,),
            in_specs=[
                pl.BlockSpec((block, width), row_map),
                pl.BlockSpec((block, pool.shape[1]), row_map),
                pl.BlockSpec((block, 1), row_map),
            ]
            + [any_spec()] * (len(pair_a) + len(pair_b)),
            out_specs=pl.BlockSpec((block, cols), lambda i, ia, ib, s: (i, 0)),
            scratch_shapes=[
                pltpu.VMEM((width, cols), BF16),
                pltpu.VMEM((pool.shape[1], cols), BF16),
                pltpu.SemaphoreType.DMA((2, pieces)),
            ],
        ),
        out_shape=jax.ShapeDtypeStruct((count, cols), BF16),
        compiler_params=params(1),
        cost_estimate=cost(2 * count * cols * (width + pool.shape[1])),
        name=name,
    )(index_a, index_b, (start // block).reshape(1), mix, pool, scale, *pair_a, *pair_b)


def incoming(final, log_total, sign):
    count = lax.axis_size("sp")

    def moved(x, step):
        pairs = [(i, i + step * sign) for i in range(count) if 0 <= i + step * sign < count]
        return lax.ppermute(x, "sp", pairs)

    wide = lambda logs: jnp.exp(logs)[:, None, :]
    covered = 1
    log_received = moved(log_total, 1)
    received = moved(final.astype(BF16), 1).astype(F32)
    while covered < count - 1:
        reach = covered + 1
        joined = (final + wide(log_total) * received).astype(BF16)
        more = moved(joined, reach).astype(F32)
        received = received + wide(log_received) * more
        if 2 * covered + 1 < count - 1:
            log_received = log_received + moved(log_total + log_received, reach)
        covered = 2 * covered + 1
    return received


def local(
    tokens,
    norm_gain,
    w_gate,
    w_value,
    w_bkey,
    w_query,
    w_pool_in,
    w_step,
    step_bias,
    decay_rate,
    decay_shift,
    conv_value,
    conv_bkey,
    conv_query,
    mix_gain,
    pool_mix,
    pool_gain,
    w_out_ssd,
    w_out_pool,
):
    tp_count = lax.axis_size("tp")
    sp_count = lax.axis_size("sp")
    fs_count = lax.axis_size("fs")
    tp_rank = lax.axis_index("tp")
    sp_rank = lax.axis_index("sp")
    heads = DUALITY_HEADS // tp_count
    groups = GROUPS // tp_count
    per_group = heads // groups
    pools = POOL_GROUPS // tp_count
    width_ssd = heads * HEAD_DIM
    width_key = groups * STATE
    width_pool = pools * POOL_DIM
    swap = [(0, 1), (1, 0)]

    bits = [1 << n for n in range(fs_count.bit_length() - 1)]
    ahead = piece_sources(bits)
    behind = piece_sources(bits[::-1])
    middle = w_bkey.shape[0] // 2
    key_pieces = gather_two(w_bkey[:middle], w_bkey[middle:])
    query_pieces, value_pieces = gather_two(w_query, w_value)
    pool_pieces, gate_pieces = gather_two(w_pool_in, w_gate)
    if w_out_ssd.shape[1] % 128 == 0:
        ssd_out_pieces, pool_out_pieces = gather_two(w_out_ssd, w_out_pool)
        out_indexes = (ahead, behind)
    else:
        joined = lambda w: (lax.all_gather(w, ("sp", "fs"), axis=1, tiled=True)[None],)
        ssd_out_pieces, pool_out_pieces = joined(w_out_ssd), joined(w_out_pool)
        out_indexes = (jnp.zeros((1,), jnp.int32),) * 2

    widened = tokens[0].astype(F32)
    scaling = lax.rsqrt(jnp.mean(widened * widened, axis=-1, keepdims=True) + EPSILON)
    own = (widened * scaling * norm_gain).astype(BF16)
    if tp_count == 2:
        other = lax.ppermute(own, "tp", swap)
        normed = jnp.concatenate(
            [jnp.where(tp_rank == 0, own, other), jnp.where(tp_rank == 0, other, own)], axis=0
        )
    else:
        normed = lax.all_gather(own, "tp", axis=0, tiled=True)
    length = normed.shape[0]
    before = lax.ppermute(normed[-REACH:], "sp", [(i, i + 1) for i in range(sp_count - 1)])
    after = lax.ppermute(normed[:REACH], "sp", [(i + 1, i) for i in range(sp_count - 1)])
    padded = jnp.concatenate([before, normed, after], axis=0)

    blocks = length // SPAN
    step_cols = lax.dynamic_slice_in_dim(w_step, tp_rank * heads, heads, 2)
    step_cols = step_cols.reshape(w_step.shape[0], 2 * heads)
    raw_steps = jnp.dot(normed, step_cols, preferred_element_type=F32)
    bias_dev = lax.dynamic_slice_in_dim(step_bias, tp_rank * heads, heads, 1)
    rate_dev = lax.dynamic_slice_in_dim(decay_rate, tp_rank * heads, heads, 1)
    steps = jax.nn.softplus(raw_steps.reshape(length, 2, heads) + bias_dev).transpose(1, 2, 0)
    logs = -rate_dev[:, :, None] * steps - decay_shift[0].transpose(1, 0, 2)
    by_span = logs.reshape(2 * heads * blocks, SPAN)
    place = jnp.arange(SPAN, dtype=jnp.int32)
    upto = (place[:, None] <= place[None, :]).astype(F32)
    inclusive = jnp.dot(by_span, upto, precision=HIGHEST).reshape(2, heads, blocks, SPAN)
    own_logs = logs.reshape(2, heads, blocks, SPAN)
    totals = inclusive[..., -1]
    forward_at = inclusive[0]
    backward_at = inclusive[1] - own_logs[1]
    backward_total = totals[1][..., None]
    flat = lambda x: x.reshape(heads, length)
    rows = jnp.concatenate([flat(forward_at), flat(backward_at), steps[0], steps[1]], axis=0)
    columns = jnp.concatenate(
        [
            flat(forward_at),
            flat(backward_at),
            flat(jnp.exp(forward_at)),
            flat(jnp.exp(backward_total - backward_at)),
        ],
        axis=0,
    ).T
    end_weights = jnp.stack(
        [
            flat(jnp.exp(totals[0][..., None] - forward_at)) * steps[0],
            flat(jnp.exp(backward_at)) * steps[1],
        ]
    )
    end_columns = (
        end_weights.reshape(2, groups, per_group, length)
        .transpose(1, 3, 0, 2)
        .reshape(groups, length, 2 * per_group)
    )

    def over_lanes(x):
        n = x.shape[-1]
        x = x.reshape(2, groups, per_group, n).transpose(1, 3, 0, 2)
        x = jnp.broadcast_to(x[..., None], (*x.shape, HEAD_DIM))
        return x.reshape(groups, n, 2 * per_group * HEAD_DIM)

    decay = over_lanes(jnp.exp(totals))
    running = jnp.cumsum(totals, axis=-1)
    entry_logs = jnp.stack([running[0] - totals[0], running[1][:, -1:] - running[1]])
    entry = over_lanes(jnp.exp(entry_logs)).transpose(1, 0, 2)
    device_logs = over_lanes(running[:, :, -1:])[:, 0]
    half = per_group * HEAD_DIM

    taps_of = lambda taps, width: lax.dynamic_slice_in_dim(
        taps, tp_rank * width, width, 1
    ).astype(F32)
    keys = convolved(
        padded, taps_of(conv_bkey, width_key), [ahead, behind], list(key_pieces), "key_conv"
    )
    queries = convolved(
        padded, taps_of(conv_query, width_key), [ahead], [query_pieces], "query_conv"
    )
    values = convolved(
        padded, taps_of(conv_value, width_ssd), [behind], [value_pieces], "value_conv"
    )
    prior, finals = block_states(keys, values, end_columns, decay)
    forward_in = incoming(finals[0], device_logs[:, :half], 1)
    backward_in = incoming(finals[1], device_logs[:, half:], -1)

    where = jnp.stack(
        [sp_rank * length, jnp.int32(length * sp_count), tp_rank * pools]
    ).astype(jnp.int32)
    pool_out = pool_branch(
        padded,
        ahead,
        pool_pieces,
        where,
        lax.dynamic_slice_in_dim(pool_mix, tp_rank * pools, pools, 0),
        lax.dynamic_slice_in_dim(pool_gain, tp_rank * width_pool, width_pool, 0)[None],
    )
    gate = gate_projection(padded, behind, gate_pieces)
    gain_dev = lax.dynamic_slice_in_dim(mix_gain, tp_rank * width_ssd, width_ssd, 0)[None]
    ssd_mix, squares = mixed_heads(
        queries,
        keys,
        values,
        gate,
        prior,
        forward_in,
        backward_in,
        entry,
        columns,
        rows,
        gain_dev,
        heads,
    )
    if tp_count == 2:
        squares = squares + lax.ppermute(squares, "tp", swap)
    else:
        squares = lax.psum(squares, "tp")
    scale = lax.rsqrt(squares / D_SSM + EPSILON)
    project = functools.partial(
        output_rows, ssd_mix, pool_out, scale, *out_indexes, ssd_out_pieces, pool_out_pieces
    )
    if tp_count == 2:
        part = length // 2
        sent = project((1 - tp_rank) * part, part, "out_other")
        received = lax.ppermute(sent, "tp", swap)
        kept = project(tp_rank * part, part, "out_own")
        summed = (kept.astype(F32) + received.astype(F32)).astype(BF16)
    else:
        partial = project(jnp.int32(0), length, "out_all")
        summed = lax.psum_scatter(partial, "tp", scatter_dimension=0, tiled=True)
    return summed[None]


def solution(mesh):
    return jax.shard_map(
        local,
        mesh=mesh,
        in_specs=(
            P("fs", ("sp", "tp"), None),
            P(),
            P(("sp", "fs"), "tp"),
            P(("sp", "fs"), "tp"),
            P(("sp", "fs"), "tp"),
            P(("sp", "fs"), "tp"),
            P(("sp", "fs"), "tp"),
            P(),
            P(),
            P(),
            P("fs", "tp", None, "sp"),
            P(),
            P(),
            P(),
            P(),
            P(),
            P(),
            P("tp", ("sp", "fs")),
            P("tp", ("sp", "fs")),
        ),
        out_specs=P("fs", ("sp", "tp"), None),
        check_vma=False,
    )
```
